32 devices in a mesh: fs: 8 (over z, x), tp: 4 (over y, core).
Axes of the slice: x: 2, y: 2, z: 4, core: 2. Of those that a mesh axis runs over, the one named last changes fastest.
Arguments:
- tokens: bfloat16 [1536, 2048], P('fs'), may hold values from -6 to 6
- norm_gain: float32 [2048], P('fs'), may hold values from 0.1 to 1.9
- expert_gate: float32 [16, 2048, 1024], P(None, 'fs', 'tp'), may hold values from -0.125 to 0.125
- expert_up: float32 [16, 2048, 1024], P(None, 'fs', 'tp'), may hold values from -0.125 to 0.125
- expert_down: float32 [16, 1024, 2048], P(None, 'fs', 'tp'), may hold values from -0.1875 to 0.1875
- shared_gate: float32 [2048, 1024], P('fs', 'tp'), may hold values from -0.125 to 0.125
- shared_up: float32 [2048, 1024], P('fs', 'tp'), may hold values from -0.125 to 0.125
- shared_down: float32 [1024, 2048], P('fs', 'tp'), may hold values from -0.1875 to 0.1875
- expert_ids: int32 [1536, 8], P('fs'), may hold values from 0 to 15, all different within a row; in each aligned block of 192 rows (0 to 191, 192 to 383, ...) at most 192 rows name the same one
- route_weights: float32 [1536, 8], P('fs'), may hold values from 0.25 to 1
Outputs:
- gate_ready: bfloat16 [16, 2048, 1024], P('fs', None, 'tp')
- up_ready: bfloat16 [16, 2048, 1024], P('fs', None, 'tp')
- down_ready: bfloat16 [16, 1024, 2048], P('fs', None, 'tp')
- shared_gate_ready: bfloat16 [2048, 1024], P(None, 'tp')
- shared_up_ready: bfloat16 [2048, 1024], P(None, 'tp')
- shared_down_ready: bfloat16 [1024, 2048], P(None, 'tp')
- mixed: bfloat16 [1536, 2048], P('fs', 'tp')
The draws below stay inside these ranges and needn't reach their ends.
Inputs may be any that keep to these rules, and one draw needn't show every extreme that they name: `expert_ids`: each row names 8 different experts. Among the 192 rows of one index of fs no expert is named more than 192 times, and in every draw some expert is named exactly 192 times there.
All inputs are finite; a program needn't handle non-finite values.
Results may differ from the reference program's by a relative error of at most 0.0085.
Values may be sent and summed in bfloat16 or wider, within the bound.
A program may use at most 128 MiB of HBM per device.

```python
import math
import jax
import jax.numpy as jnp
import numpy as np
from jax import lax

D = 2048
DE = 1024
TOP_K = 8
TOK_DEV = 192
EXPERTS = 16
TOKENS = 1536
CAPE = 192
N_FS = 8


def steps_of(own_key, extent, pieces, low, top_value):
    level, own = 1.0, jax.random.fold_in(own_key, 6)
    for axis_at, parts in pieces:
        draws = jnp.exp(jax.random.uniform(jax.random.fold_in(own, axis_at), (parts,), jnp.float32, low / len(pieces), top_value / len(pieces)))
        level = level * jnp.repeat(draws, extent[axis_at] // parts).reshape([-1 if axis == axis_at else 1 for axis in range(len(extent))])
    return level


def routed_block(key, own, number, rows, count, top, limit, slope):
    ranking = jax.random.permutation(key, count)
    crowded, common = shares(count, rows * top, limit, slope, True), shares(count, rows * top, limit, slope, False)
    places = jnp.arange(count)

    def named(tallies, offset_by):
        used = int((tallies > 0).sum())
        fixed = max(1, used // 4)
        moved = fixed + (places - fixed + offset_by * (used - fixed)) % max(1, count - fixed)
        return jnp.zeros((count,), jnp.int32).at[ranking[jnp.where(places < fixed, places, moved)]].set(jnp.asarray(tallies, jnp.int32))

    tallies = jnp.where(number % 4 == 0, named(crowded, number // 4), named(common, number - number // 4 - 1))
    mixed = jax.random.permutation(jax.random.fold_in(own, 3), count)
    giver, receiver = mixed[0:count // 2 * 2:2], mixed[1:count // 2 * 2:2]
    slack = jnp.minimum(tallies[giver] - 1, limit - tallies[receiver]) // 2
    slack = jnp.where((giver == ranking[0]) | (receiver == ranking[0]) | (tallies[receiver] == 0), 0, jnp.maximum(slack, 0))
    moved = jax.random.randint(jax.random.fold_in(own, 4), (count // 2,), 0, 1 << 20) % (slack + 1)
    tallies = tallies.at[giver].add(-moved).at[receiver].add(moved)
    members = jnp.searchsorted(jnp.cumsum(tallies), jnp.arange(rows * top), side="right").astype(jnp.int32)
    grid = members.reshape(top, rows).T
    grid = grid[jax.random.permutation(jax.random.fold_in(own, 1), rows)]
    offset_by = jax.random.randint(jax.random.fold_in(own, 2), (rows, 1), 0, top)
    return jnp.take_along_axis(grid, (jnp.arange(top)[None, :] + offset_by) % top, axis=1)


def shares(count, total, bound, lean, full):
    portions = [(1 << 20) // math.isqrt(rank ** lean) + 1 for rank in range(1, count + 1)]
    largest = bound if full else min(bound, max(-(-total // count), total * portions[0] // sum(portions)))
    least = 1 if total - largest >= count - 1 else 0
    counts, spare = [largest] + [least] * (count - 1), total - largest - least * (count - 1)
    while spare > 0:
        candidates = [i for i in range(1, count) if counts[i] < largest] or [i for i in range(1, count) if counts[i] < bound]
        pool, remaining = sum([portions[i] for i in candidates]), spare
        for i in candidates:
            more = min(bound - counts[i], max(1, remaining * portions[i] // pool), spare)
            counts[i] = counts[i] + more
            spare = spare - more
    return np.array(counts)


def scatter_about(own_key, dims, spread, reach, cuts=(), kind=jnp.bfloat16):
    values = spread * jax.random.normal(own_key, dims, jnp.float32)
    if cuts:
        values = values * steps_of(own_key, dims, cuts, -0.22, 0.18)
    return jnp.clip(values, -reach, reach).astype(kind)


def setup_inputs(seed: int = 0) -> dict:
    arg_keys = jax.random.split(jax.random.key(seed), 11)
    tokens = scatter_about(arg_keys[0], (TOKENS, D), 1.0, 6.0, ((0, 8),))
    norm_gain = jnp.clip(1.0 + 0.18 * jax.random.normal(arg_keys[1], (D,), jnp.float32), 0.1, 1.9)
    expert_gate = scatter_about(arg_keys[2], (EXPERTS, D, DE), D ** -0.5, 0.125, ((1, 8), (2, 4)), jnp.float32)
    expert_up = scatter_about(arg_keys[3], (EXPERTS, D, DE), D ** -0.5, 0.125, ((1, 8), (2, 4)), jnp.float32)
    expert_down = scatter_about(arg_keys[4], (EXPERTS, DE, D), DE ** -0.5, 0.1875, ((1, 8), (2, 4)), jnp.float32)
    shared_gate = scatter_about(arg_keys[5], (D, DE), D ** -0.5, 0.125, ((0, 8), (1, 4)), jnp.float32)
    shared_up = scatter_about(arg_keys[6], (D, DE), D ** -0.5, 0.125, ((0, 8), (1, 4)), jnp.float32)
    shared_down = scatter_about(arg_keys[7], (DE, D), DE ** -0.5, 0.1875, ((0, 8), (1, 4)), jnp.float32)
    expert_ids_keys = jax.random.split(jax.random.fold_in(arg_keys[8], 1), TOKENS // TOK_DEV)
    expert_ids_turns = jax.random.permutation(jax.random.fold_in(arg_keys[8], 3), TOKENS // TOK_DEV)
    expert_ids = jax.vmap(lambda own, number: routed_block(jax.random.fold_in(arg_keys[8], 2), own, number, TOK_DEV, EXPERTS, TOP_K, CAPE, 1))(expert_ids_keys, expert_ids_turns).reshape((TOKENS, TOP_K))
    route_weights = jnp.clip(jnp.exp(math.log(1.0) - 1.3862944 * jax.random.uniform(arg_keys[9], (TOKENS, TOP_K), jnp.float32) ** steps_of(arg_keys[9], (TOKENS, TOP_K), ((0, 8),), -0.2, 0.2)), 0.25, 1.0)
    return {"tokens": tokens, "norm_gain": norm_gain, "expert_gate": expert_gate, "expert_up": expert_up, "expert_down": expert_down, "shared_gate": shared_gate, "shared_up": shared_up, "shared_down": shared_down, "expert_ids": expert_ids, "route_weights": route_weights}


EPS = 1e-06

def reference(tokens, norm_gain, expert_gate, expert_up, expert_down, shared_gate, shared_up, shared_down, expert_ids, route_weights):
    gain = norm_gain.astype(jnp.float32)
    gate_ready = (expert_gate * gain[None, :, None]).astype(jnp.bfloat16)
    up_ready = (expert_up * gain[None, :, None]).astype(jnp.bfloat16)
    down_ready = expert_down.astype(jnp.bfloat16)
    shared_gate_ready = (shared_gate * gain[:, None]).astype(jnp.bfloat16)
    shared_up_ready = (shared_up * gain[:, None]).astype(jnp.bfloat16)
    shared_down_ready = shared_down.astype(jnp.bfloat16)
    wide = tokens.astype(jnp.float32)
    normed = (wide * lax.rsqrt(lax.optimization_barrier(jnp.mean(wide * wide, axis=-1, keepdims=True)) + EPS)).astype(jnp.bfloat16)
    shared_first = jnp.dot(normed, shared_gate_ready, preferred_element_type=jnp.float32)
    shared_second = jnp.dot(normed, shared_up_ready, preferred_element_type=jnp.float32)
    shared_hidden = (jax.nn.silu(shared_first) * shared_second).astype(jnp.bfloat16)
    shared_out = jnp.dot(shared_hidden, shared_down_ready, preferred_element_type=jnp.float32)
    experts = expert_gate.shape[0]
    tok_block = tokens.shape[0] // N_FS
    capacity = 2 * tok_block * TOP_K // experts
    chosen = expert_ids.reshape(N_FS, tok_block * TOP_K).astype(jnp.int32)
    onehot = (chosen[..., None] == jnp.arange(experts, dtype=jnp.int32)).astype(jnp.int32)
    ranks = (lax.optimization_barrier(jnp.sum(jnp.cumsum(onehot, axis=1) * onehot, axis=-1)) - 1).astype(jnp.int32)
    blocks = jnp.broadcast_to(jnp.arange(N_FS, dtype=jnp.int32)[:, None], chosen.shape)
    owners = (blocks * tok_block + jnp.arange(tok_block * TOP_K, dtype=jnp.int32)[None, :] // TOP_K).astype(jnp.int32)
    slot_token = jnp.zeros((experts, N_FS, capacity), jnp.int32).at[chosen, blocks, ranks].set(owners)
    slot_weight = jnp.zeros((experts, N_FS, capacity), jnp.float32).at[chosen, blocks, ranks].set(route_weights.reshape(N_FS, -1).astype(jnp.float32))

    def one_expert(total, index):
        which = slot_token[index].reshape(-1)
        rows = normed[which]
        first = jnp.dot(rows, gate_ready[index], preferred_element_type=jnp.float32)
        second = jnp.dot(rows, up_ready[index], preferred_element_type=jnp.float32)
        hidden = (jax.nn.silu(first) * second).astype(jnp.bfloat16)
        result = jnp.dot(hidden, down_ready[index], preferred_element_type=jnp.float32).astype(jnp.bfloat16)
        result = lax.optimization_barrier(result).astype(jnp.float32)
        return (total.at[which].add(result * slot_weight[index].reshape(-1)[:, None]), None)
    routed, _ = lax.scan(one_expert, jnp.zeros(tokens.shape, jnp.float32), jnp.arange(experts, dtype=jnp.int32))
    mixed = (shared_out + routed).astype(jnp.bfloat16)
    return (gate_ready, up_ready, down_ready, shared_gate_ready, shared_up_ready, shared_down_ready, mixed)
```

```python
import functools
import jax
import jax.numpy as jnp
from jax import lax
from jax.experimental import pallas as pl
from jax.experimental.pallas import tpu as pltpu
from jax.sharding import PartitionSpec as P

TOP_K = 8


EPS = 1e-06

MESH = pl.DeviceIdType.MESH
LANES = 128


def flip(value, mask, extent):
    result, bit = 0, 1
    while bit < extent:
        digit = (value // bit) % 2
        result = result + bit * ((1 - digit) if mask & bit else digit)
        bit *= 2
    return result


def fused_kernel(
    groups,
    ranks,
    ext,
    gain,
    eg,
    eu,
    ed,
    sg,
    su,
    sd,
    out_g,
    out_u,
    out_d,
    out_sg,
    out_su,
    out_sd,
    out_mixed,
    st_g,
    st_u,
    st_d,
    sb_g,
    sb_u,
    sb_d,
    rv_g,
    rv_u,
    rv_d,
    sh,
    tok,
    hid,
    shid,
    res_s,
    res_r,
    own_out,
    load_sem,
    loc_sem,
    a2a_send,
    a2a_recv,
    tok_send,
    tok_recv,
    tok_csend,
    tok_crecv,
    sh_send,
    sh_recv,
    hid_csend,
    hid_ysend,
    hid_fsend,
    hid_recv,
    shid_send,
    shid_recv,
    res_send,
    res_recv,
    out_sem,
    shout_sem,
):
    nx = 2
    nz = groups // nx
    me = lax.axis_index("fs")
    tp = lax.axis_index("tp")
    z, x = me // nx, me % nx
    core = tp % 2
    partner = flip(tp, 1, ranks)
    across = flip(tp, 2, ranks)
    per = eg.shape[0] // groups
    experts = eg.shape[0]
    rows_w = eg.shape[1]
    rows_d = ed.shape[1]
    tok_count = ext.shape[0]
    width = st_d.shape[2] * ranks
    half = tok_count // 2
    hcols = eg.shape[2]
    dcols = ed.shape[2]
    hw = dcols // 2

    loads = [
        pltpu.make_async_copy(a, b, load_sem.at[i])
        for i, (a, b) in enumerate(((eg, st_g), (eu, st_u), (ed, st_d)))
    ]
    for load in loads:
        load.start()
    own_tok = pltpu.make_async_copy(ext, tok.at[me], loc_sem.at[3])
    own_tok.start()

    barrier = pltpu.get_barrier_semaphore()
    for o in range(1, groups):
        pl.semaphore_signal(
            barrier, inc=1, device_id={"fs": flip(me, o, groups)}, device_id_type=MESH
        )
    for o in range(1, ranks):
        pl.semaphore_signal(
            barrier, inc=1, device_id={"tp": flip(tp, o, ranks)}, device_id_type=MESH
        )
    pl.semaphore_wait(barrier, groups + ranks - 2)

    mine = pl.ds(core * half, half)
    theirs = pl.ds((1 - core) * half, half)

    def fs_copy(src, dst, send, recv, target):
        return pltpu.make_async_remote_copy(
            src_ref=src,
            dst_ref=dst,
            send_sem=send,
            recv_sem=recv,
            device_id={"fs": target},
            device_id_type=MESH,
        )

    def tp_copy(src, dst, send, recv, target):
        return pltpu.make_async_remote_copy(
            src_ref=src,
            dst_ref=dst,
            send_sem=send,
            recv_sem=recv,
            device_id={"tp": target},
            device_id_type=MESH,
        )

    def tok_copy(block, slot, target, own=False):
        src = ext.at[mine] if own else tok.at[block, mine]
        return fs_copy(src, tok.at[block, mine], tok_send.at[slot], tok_recv.at[block], target)

    def sh_copy(block, slot, target, own=False):
        return fs_copy(sh.at[block], sh.at[block], sh_send.at[slot], sh_recv.at[block], target)

    def gather_moves(copy, recv_copy, step, act):
        other = 1 - x
        if step == 0:

            @pl.when(z + 1 < nz)
            def _():
                act(copy(me, 0, me + nx, True))

            @pl.when(z >= 1)
            def _():
                act(copy(me, 1, me - nx, True))

            act(copy(me, 2, z * nx + other, True))
            return

        @pl.when(z >= step)
        def _():
            block = me - step * nx
            recv_copy(block)

            @pl.when(z + 1 < nz)
            def _():
                act(copy(block, 4 * step - 1, me + nx))

            act(copy(block, 4 * step, z * nx + other))

        @pl.when(z + step < nz)
        def _():
            block = me + step * nx
            recv_copy(block)

            @pl.when(z >= 1)
            def _():
                act(copy(block, 4 * step + 1, me - nx))

            act(copy(block, 4 * step + 2, z * nx + other))

    def start(c):
        c.start()

    def wait_send(c):
        c.wait_send()

    def nothing(block):
        pass

    def tok_arrive(block):
        tok_copy(block, 0, me).wait_recv()
        core_copy(block).start()

    def core_copy(block):
        return tp_copy(
            tok.at[block, mine],
            tok.at[block, mine],
            tok_csend.at[block],
            tok_crecv.at[block],
            partner,
        )

    def sh_arrive(block):
        sh_copy(block, 0, me).wait_recv()

    gather_moves(tok_copy, nothing, 0, start)

    column = gain[...]
    sh[me, 0] = (sg[...] * column).astype(jnp.bfloat16)
    sh[me, 1] = (su[...] * column).astype(jnp.bfloat16)
    sh[me, 2, 0:rows_d] = sd[:, 0:hw].astype(jnp.bfloat16)
    sh[me, 2, rows_d : 2 * rows_d] = sd[:, hw:dcols].astype(jnp.bfloat16)

    def cast(stage, sendbuf, scaled):
        @pl.loop(0, experts)
        def _(e):
            value = stage[e]
            if scaled:
                value = value * gain[...]
            sendbuf[e] = value.astype(jnp.bfloat16)

    order = [o for o in (6, 4, 2, 7, 5, 3, 1) if o < groups]
    order = order + [o for o in range(1, groups) if o not in order]

    def a2a_copy(index, o):
        sendbuf, recvbuf, rows = (
            (sb_g, rv_g, rows_w),
            (sb_u, rv_u, rows_w),
            (sb_d, rv_d, rows_d),
        )[index]
        target = flip(me, o, groups)
        return fs_copy(
            sendbuf.at[pl.ds(target * per, per)],
            recvbuf.at[:, pl.ds(me * rows, rows), :],
            a2a_send.at[index, o],
            a2a_recv.at[index, o],
            target,
        )

    def a2a_own(index):
        sendbuf, recvbuf, rows = (
            (sb_g, rv_g, rows_w),
            (sb_u, rv_u, rows_w),
            (sb_d, rv_d, rows_d),
        )[index]
        return pltpu.make_async_copy(
            sendbuf.at[pl.ds(me * per, per)],
            recvbuf.at[:, pl.ds(me * rows, rows), :],
            loc_sem.at[index],
        )

    def a2a_start(index):
        for o in order:
            a2a_copy(index, o).start()
        a2a_own(index).start()

    def a2a_arrive(index, recvbuf, out):
        for o in order:
            a2a_copy(index, o).wait_recv()
        a2a_own(index).wait()
        pltpu.make_async_copy(recvbuf, out, out_sem.at[index]).start()

    loads[0].wait()
    cast(st_g, sb_g, True)
    gather_moves(sh_copy, nothing, 0, start)
    gather_moves(tok_copy, tok_arrive, 1, start)
    a2a_start(0)
    loads[1].wait()
    cast(st_u, sb_u, True)
    gather_moves(sh_copy, sh_arrive, 1, start)
    for step in range(2, nz):
        gather_moves(tok_copy, tok_arrive, step, start)
        if step == 2:
            a2a_start(1)
            loads[2].wait()
            cast(st_d, sb_d, False)
        gather_moves(sh_copy, sh_arrive, step, start)
    a2a_start(2)

    for zz in range(nz):
        tok_arrive(zz * nx + (1 - x))
    for zz in range(nz):
        sh_arrive(zz * nx + (1 - x))
    own_tok.wait()

    def sh_out(block, part):
        src_dst = (
            (sh.at[block, 0], out_sg.at[pl.ds(block * rows_w, rows_w), :]),
            (sh.at[block, 1], out_su.at[pl.ds(block * rows_w, rows_w), :]),
            (sh.at[block, 2, pl.ds(0, rows_d)], out_sd.at[pl.ds(block * rows_d, rows_d), pl.ds(0, hw)]),
            (sh.at[block, 2, pl.ds(rows_d, rows_d)], out_sd.at[pl.ds(block * rows_d, rows_d), pl.ds(hw, hw)]),
        )[part]
        return pltpu.make_async_copy(*src_dst, shout_sem.at[block, part])

    for block in range(groups):
        for part in range(4):
            sh_out(block, part).start()

    features = groups * rows_w

    def shared_half(part):
        total = jnp.zeros((tok_count, hcols), jnp.float32)
        for block in range(groups):
            total = total + jnp.dot(
                ext[:, block * rows_w : (block + 1) * rows_w],
                sh[block, part],
                preferred_element_type=jnp.float32,
            )
        return total

    shared_first = shared_half(0)
    shared_second = shared_half(1)
    shid[tp] = (jax.nn.silu(shared_first) * shared_second).astype(jnp.bfloat16)

    def shid_copy(o):
        return tp_copy(
            shid.at[tp], shid.at[tp], shid_send.at[o], shid_recv.at[o], flip(tp, o, ranks)
        )

    def core_arrive(block):
        tp_copy(
            tok.at[block, theirs],
            tok.at[block, theirs],
            tok_csend.at[block],
            tok_crecv.at[block],
            partner,
        ).wait_recv()

    for o in range(1, groups):
        core_arrive(flip(me, o, groups))

    for o in range(1, ranks):
        shid_copy(o).start()

    a2a_arrive(0, rv_g, out_g)
    a2a_arrive(1, rv_u, out_u)

    def hid_core(block):
        return tp_copy(
            hid.at[tp, block], hid.at[tp, block], hid_csend.at[block], hid_recv.at[1, block], partner
        )

    def hid_across(block):
        return tp_copy(
            hid.at[tp, block], hid.at[tp, block], hid_ysend.at[block], hid_recv.at[2, block], across
        )

    def hid_forward(block):
        return tp_copy(
            hid.at[across, block],
            hid.at[across, block],
            hid_fsend.at[block],
            hid_recv.at[3, block],
            partner,
        )

    def turn(o):
        return (me + o) % groups

    @pl.loop(0, groups)
    def _(o):
        block = turn(o + 1)
        rows = tok[block, :, 0:features]
        for e in range(per):
            first = jnp.dot(rows, rv_g[e], preferred_element_type=jnp.float32)
            second = jnp.dot(rows, rv_u[e], preferred_element_type=jnp.float32)
            hid[tp, block, e] = (jax.nn.silu(first) * second).astype(jnp.bfloat16)

        @pl.when(o >= 1)
        def _():
            before = turn(o)
            hid_across(before).start()
            hid_core(before).start()

    for o in range(1, ranks):
        shid_copy(o).wait_recv()
    hid_across(me).start()
    hid_core(me).start()
    for part in range(2):
        total = jnp.zeros((tok_count, hw), jnp.float32)
        for block in range(groups):
            at = block * rows_d
            total = total + jnp.dot(
                shid[at // hcols, :, at % hcols : at % hcols + rows_d],
                sh[block, 2, part * rows_d : (part + 1) * rows_d],
                preferred_element_type=jnp.float32,
            )
        own_out[:, part * hw : (part + 1) * hw] = total

    @pl.loop(0, groups)
    def _(o):
        block = turn(o + 1)
        hid_across(block).wait_recv()
        hid_forward(block).start()

    a2a_arrive(2, rv_d, out_d)

    lanes = lax.broadcasted_iota(jnp.int32, (tok_count, LANES), 1)

    def res_copy(o):
        target = turn(o)
        return fs_copy(
            res_s.at[target], res_r.at[me], res_send.at[o], res_recv.at[o], target
        )

    def block_out(block):
        table = tok[block, :, features : features + LANES].astype(jnp.float32)
        total = jnp.zeros((tok_count, dcols), jnp.float32)
        for e in range(per):
            expert = me * per + e
            weight = jnp.sum(
                jnp.where(
                    (lanes == expert) | (lanes == expert + experts) | (lanes == expert + 2 * experts),
                    table,
                    0.0,
                ),
                axis=1,
                keepdims=True,
            )
            out = jnp.zeros((tok_count, dcols), jnp.float32)
            for r in range(ranks):
                out = out + jnp.dot(
                    hid[r, block, e],
                    rv_d[e, r * hcols : (r + 1) * hcols],
                    preferred_element_type=jnp.float32,
                )
            total = total + weight * out
        return total

    @pl.loop(1, groups + 1)
    def _(o):
        block = turn(o)
        hid_core(block).wait_recv()
        hid_forward(block).wait_recv()

        @pl.when(o < groups)
        def _():
            res_s[block] = block_out(block).astype(jnp.bfloat16)

        @pl.when(o == groups)
        def _():
            own_out[...] = own_out[...] + block_out(block)

        @pl.when(o >= 2)
        def _():
            res_copy(o - 1).start()

    for o in range(1, groups):
        res_copy(o).wait_recv()
        own_out[...] = own_out[...] + res_r[(me + groups - o) % groups].astype(jnp.float32)
    out_mixed[...] = own_out[...].astype(jnp.bfloat16)

    for o in range(1, groups):
        res_copy(o).wait_send()
    for index in range(3):
        for o in order:
            a2a_copy(index, o).wait_send()
    for step in range(nz):
        gather_moves(tok_copy, nothing, step, wait_send)
        gather_moves(sh_copy, nothing, step, wait_send)
    for o in range(1, groups):
        core_copy(flip(me, o, groups)).wait_send()
    for o in range(1, ranks):
        shid_copy(o).wait_send()

    @pl.loop(0, groups)
    def _(o):
        hid_core(o).wait_send()
        hid_across(o).wait_send()
        hid_forward(o).wait_send()

    for index, (recvbuf, out) in enumerate(((rv_g, out_g), (rv_u, out_u), (rv_d, out_d))):
        pltpu.make_async_copy(recvbuf, out, out_sem.at[index]).wait()
    for block in range(groups):
        for part in range(4):
            sh_out(block, part).wait()


def dense_body(
    tokens,
    norm_gain,
    expert_gate,
    expert_up,
    expert_down,
    shared_gate,
    shared_up,
    shared_down,
    expert_ids,
    route_weights,
):
    groups, ranks = lax.axis_size("fs"), lax.axis_size("tp")
    experts, rows_w, hcols = expert_gate.shape
    rows_d, dcols = expert_down.shape[1:]
    per = experts // groups
    tok_count, features = tokens.shape
    wide = tokens.astype(jnp.float32)
    normed = (wide * lax.rsqrt(jnp.mean(wide * wide, axis=-1, keepdims=True) + EPS)).astype(
        jnp.bfloat16
    )
    named = expert_ids[:, :, None] == jnp.arange(experts, dtype=jnp.int32)[None, None, :]
    table = jnp.sum(jnp.where(named, route_weights[:, :, None], 0.0), axis=1)
    high = lax.reduce_precision(table, 8, 7)
    middle = lax.reduce_precision(table - high, 8, 7)
    low = table - high - middle
    pad = jnp.zeros((tok_count, LANES - 3 * experts), jnp.bfloat16)
    ext = jnp.concatenate(
        [normed] + [v.astype(jnp.bfloat16) for v in (high, middle, low)] + [pad], axis=1
    )
    total = features + LANES
    bf, f32 = jnp.bfloat16, jnp.float32
    dma = pltpu.SemaphoreType.DMA
    nz = groups // 2
    any_space = pl.BlockSpec(memory_space=pl.ANY)
    vmem = pl.BlockSpec(memory_space=pltpu.VMEM)
    hidden = hcols * ranks
    return pl.pallas_call(
        functools.partial(fused_kernel, groups, ranks),
        out_shape=(
            jax.ShapeDtypeStruct((per, features, hcols), bf),
            jax.ShapeDtypeStruct((per, features, hcols), bf),
            jax.ShapeDtypeStruct((per, hidden, dcols), bf),
            jax.ShapeDtypeStruct((features, hcols), bf),
            jax.ShapeDtypeStruct((features, hcols), bf),
            jax.ShapeDtypeStruct((hidden, dcols), bf),
            jax.ShapeDtypeStruct((tok_count, dcols), bf),
        ),
        in_specs=[vmem, vmem, any_space, any_space, any_space, vmem, vmem, vmem],
        out_specs=(any_space,) * 6 + (vmem,),
        scratch_shapes=[
            pltpu.VMEM((experts, rows_w, hcols), f32),
            pltpu.VMEM((experts, rows_w, hcols), f32),
            pltpu.VMEM((experts, rows_d, dcols), f32),
            pltpu.VMEM((experts, rows_w, hcols), bf),
            pltpu.VMEM((experts, rows_w, hcols), bf),
            pltpu.VMEM((experts, rows_d, dcols), bf),
            pltpu.VMEM((per, features, hcols), bf),
            pltpu.VMEM((per, features, hcols), bf),
            pltpu.VMEM((per, hidden, dcols), bf),
            pltpu.VMEM((groups, 3, rows_w, hcols), bf),
            pltpu.VMEM((groups, tok_count, total), bf),
            pltpu.VMEM((ranks, groups, per, tok_count, hcols), bf),
            pltpu.VMEM((ranks, tok_count, hcols), bf),
            pltpu.VMEM((groups, tok_count, dcols), bf),
            pltpu.VMEM((groups, tok_count, dcols), bf),
            pltpu.VMEM((tok_count, dcols), f32),
            dma((3,)),
            dma((4,)),
            dma((3, groups)),
            dma((3, groups)),
            dma((4 * nz,)),
            dma((groups,)),
            dma((groups,)),
            dma((groups,)),
            dma((4 * nz,)),
            dma((groups,)),
            dma((groups,)),
            dma((groups,)),
            dma((groups,)),
            dma((4, groups)),
            dma((ranks,)),
            dma((ranks,)),
            dma((groups,)),
            dma((groups,)),
            dma((3,)),
            dma((groups, 4)),
        ],
        compiler_params=pltpu.CompilerParams(
            collective_id=0, has_side_effects=True, vmem_limit_bytes=60 * 1024 * 1024
        ),
    )(
        ext,
        norm_gain[:, None],
        expert_gate,
        expert_up,
        expert_down,
        shared_gate,
        shared_up,
        shared_down,
    )


def expert_hidden(rows, gate_new, up_new):
    first = jnp.einsum("secn,enf->secf", rows, gate_new, preferred_element_type=jnp.float32)
    second = jnp.einsum("secn,enf->secf", rows, up_new, preferred_element_type=jnp.float32)
    return (jax.nn.silu(first) * second).astype(jnp.bfloat16)


def body(
    tokens,
    norm_gain,
    expert_gate,
    expert_up,
    expert_down,
    shared_gate,
    shared_up,
    shared_down,
    expert_ids,
    route_weights,
):
    groups = lax.axis_size("fs")
    experts = expert_gate.shape[0]
    per_group = experts // groups
    tok_count = tokens.shape[0]
    capacity = 2 * tok_count * TOP_K // experts
    ranks = lax.axis_size("tp")
    square = expert_down.shape[1] * expert_down.shape[2] == shared_gate.size
    if capacity >= tok_count and groups & (groups - 1) == 0 and ranks == 4 and square:
        return dense_body(
            tokens,
            norm_gain,
            expert_gate,
            expert_up,
            expert_down,
            shared_gate,
            shared_up,
            shared_down,
            expert_ids,
            route_weights,
        )
    gate_local = (expert_gate * norm_gain[None, :, None]).astype(jnp.bfloat16)
    up_local = (expert_up * norm_gain[None, :, None]).astype(jnp.bfloat16)
    down_local = expert_down.astype(jnp.bfloat16)
    gate_local = gate_local.reshape((groups, per_group) + gate_local.shape[1:])
    up_local = up_local.reshape((groups, per_group) + up_local.shape[1:])
    down_local = down_local.reshape((groups, per_group) + down_local.shape[1:])
    shared_first_local = (shared_gate * norm_gain[:, None]).astype(jnp.bfloat16)
    shared_second_local = (shared_up * norm_gain[:, None]).astype(jnp.bfloat16)
    shared_third_local = shared_down.astype(jnp.bfloat16)
    gate_moved, up_moved, down_moved = (
        lax.all_to_all(gate_local, "fs", split_axis=0, concat_axis=2, tiled=True),
        lax.all_to_all(up_local, "fs", split_axis=0, concat_axis=2, tiled=True),
        lax.all_to_all(down_local, "fs", split_axis=0, concat_axis=2, tiled=True),
    )
    down_ready = down_moved[0]
    gate_ready = gate_moved[0]
    up_ready = up_moved[0]
    shared_gate_ready, shared_up_ready, shared_down_ready = (
        lax.all_gather(shared_first_local, "fs", axis=0, tiled=True),
        lax.all_gather(shared_second_local, "fs", axis=0, tiled=True),
        lax.all_gather(shared_third_local, "fs", axis=0, tiled=True),
    )
    wide = tokens.astype(jnp.float32)
    normed = (wide * lax.rsqrt(jnp.mean(wide * wide, axis=-1, keepdims=True) + EPS)).astype(
        jnp.bfloat16
    )
    chosen = expert_ids.reshape(-1)
    onehot = (chosen[:, None] == jnp.arange(experts, dtype=jnp.int32)[None, :]).astype(jnp.int32)
    ranks = jnp.sum(jnp.cumsum(onehot, axis=0) * onehot, axis=1) - 1
    owners = jnp.arange(tok_count * TOP_K, dtype=jnp.int32) // TOP_K
    slot_token = jnp.zeros((experts, capacity), jnp.int32).at[chosen, ranks].set(owners)
    outgoing = normed[slot_token.reshape(-1)].reshape(groups, per_group, capacity, normed.shape[1])
    share = capacity // lax.axis_size("tp")
    mine = lax.dynamic_slice_in_dim(outgoing, lax.axis_index("tp") * share, share, 2)
    arrived = lax.all_to_all(mine, "fs", split_axis=0, concat_axis=0, tiled=True)
    hidden = expert_hidden(lax.all_gather(arrived, "tp", axis=2, tiled=True), gate_ready, up_ready)
    shared_first = jnp.dot(normed, shared_gate_ready, preferred_element_type=jnp.float32)
    shared_second = jnp.dot(normed, shared_up_ready, preferred_element_type=jnp.float32)
    shared_hidden = (jax.nn.silu(shared_first) * shared_second).astype(jnp.bfloat16)[None, None]
    columns = down_ready.shape[2]
    routed_piece = lax.all_gather(hidden, "tp", axis=3, tiled=True)
    shared_piece = lax.all_gather(shared_hidden, "tp", axis=3, tiled=True)
    routed_total = jnp.einsum(
        "secf,efd->secd", routed_piece, down_ready, preferred_element_type=jnp.float32
    )
    shared_total = jnp.einsum(
        "abtf,fd->abtd", shared_piece, shared_down_ready, preferred_element_type=jnp.float32
    )
    returned = lax.all_to_all(
        routed_total.astype(jnp.bfloat16), "fs", split_axis=0, concat_axis=0, tiled=True
    )
    returned = returned.reshape(experts * capacity, columns)
    picked = (
        returned[chosen * capacity + ranks].astype(jnp.float32).reshape(tok_count, TOP_K, columns)
    )
    routed = jnp.sum(picked * route_weights[:, :, None], axis=1)
    mixed = (shared_total[0, 0] + routed).astype(jnp.bfloat16)
    return (
        gate_ready,
        up_ready,
        down_ready,
        shared_gate_ready,
        shared_up_ready,
        shared_down_ready,
        mixed,
    )


def solution(mesh):
    in_specs = (
        P("fs", None),
        P("fs"),
        P(None, "fs", "tp"),
        P(None, "fs", "tp"),
        P(None, "fs", "tp"),
        P("fs", "tp"),
        P("fs", "tp"),
        P("fs", "tp"),
        P("fs", None),
        P("fs", None),
    )
    out_specs = (
        P("fs", None, "tp"),
        P("fs", None, "tp"),
        P("fs", None, "tp"),
        P(None, "tp"),
        P(None, "tp"),
        P(None, "tp"),
        P("fs", "tp"),
    )
    return jax.shard_map(body, mesh=mesh, in_specs=in_specs, out_specs=out_specs, check_vma=False)
```

```python
import functools
import jax
import jax.numpy as jnp
from jax import lax
from jax.experimental import pallas as pl
from jax.experimental.pallas import tpu as pltpu
from jax.sharding import PartitionSpec as P

TOP_K = 8


EPS = 1e-06

MESH = pl.DeviceIdType.MESH
LANES = 128
VMEM_BYTES = 48 * 1024 * 1024


def flip(value, mask, extent):
    result, bit = 0, 1
    while bit < extent:
        digit = (value // bit) % 2
        result = result + bit * ((1 - digit) if mask & bit else digit)
        bit *= 2
    return result


def fused_kernel(
    groups,
    ranks,
    ext,
    gain,
    eg,
    eu,
    ed,
    sg,
    su,
    sd,
    rv_g,
    rv_u,
    rv_d,
    out_sg,
    out_su,
    out_sd,
    out_mixed,
    st_g,
    st_u,
    st_d,
    sb_g,
    sb_u,
    sb_d,
    sh,
    tok,
    hid,
    shid,
    xs,
    xr,
    zs,
    zr,
    own_out,
    load_sem,
    loc_sem,
    own_sem,
    a2a_send,
    a2a_recv,
    tok_send,
    tok_recv,
    tok_csend,
    tok_crecv,
    sh_send,
    sh_recv,
    hid_csend,
    hid_ysend,
    hid_fsend,
    hid_recv,
    shid_send,
    shid_recv,
    x_send,
    x_recv,
    z_send,
    z_recv,
    shout_sem,
):
    nx = 2
    nz = groups // nx
    me = lax.axis_index("fs")
    tp = lax.axis_index("tp")
    z, x = me // nx, me % nx
    core = tp % 2
    partner = flip(tp, 1, ranks)
    across = flip(tp, 2, ranks)
    per = eg.shape[0] // groups
    experts = eg.shape[0]
    rows_w = eg.shape[1]
    rows_d = ed.shape[1]
    tok_count = ext.shape[0]
    width = st_d.shape[2] * ranks
    half = tok_count // 2
    hcols = eg.shape[2]
    dcols = ed.shape[2]
    hw = dcols // 2

    loads = [
        pltpu.make_async_copy(a, b, load_sem.at[i])
        for i, (a, b) in enumerate(((eg, st_g), (eu, st_u), (ed, st_d)))
    ]
    for load in loads:
        load.start()
    own_tok = pltpu.make_async_copy(ext, tok.at[me], loc_sem)
    own_tok.start()

    barrier = pltpu.get_barrier_semaphore()
    for o in range(1, groups):
        pl.semaphore_signal(
            barrier, inc=1, device_id={"fs": flip(me, o, groups)}, device_id_type=MESH
        )
    for o in range(1, ranks):
        pl.semaphore_signal(
            barrier, inc=1, device_id={"tp": flip(tp, o, ranks)}, device_id_type=MESH
        )
    pl.semaphore_wait(barrier, groups + ranks - 2)

    mine = pl.ds(core * half, half)
    theirs = pl.ds((1 - core) * half, half)

    def fs_copy(src, dst, send, recv, target):
        return pltpu.make_async_remote_copy(
            src_ref=src,
            dst_ref=dst,
            send_sem=send,
            recv_sem=recv,
            device_id={"fs": target},
            device_id_type=MESH,
        )

    def tp_copy(src, dst, send, recv, target):
        return pltpu.make_async_remote_copy(
            src_ref=src,
            dst_ref=dst,
            send_sem=send,
            recv_sem=recv,
            device_id={"tp": target},
            device_id_type=MESH,
        )

    def tok_copy(block, slot, target, own=False):
        src = ext.at[mine] if own else tok.at[block, mine]
        return fs_copy(src, tok.at[block, mine], tok_send.at[slot], tok_recv.at[block], target)

    def sh_copy(block, slot, target, own=False):
        return fs_copy(sh.at[block], sh.at[block], sh_send.at[slot], sh_recv.at[block], target)

    def gather_moves(copy, recv_copy, step, act):
        other = 1 - x
        if step == 0:

            @pl.when(z + 1 < nz)
            def _():
                act(copy(me, 0, me + nx, True))

            @pl.when(z >= 1)
            def _():
                act(copy(me, 1, me - nx, True))

            act(copy(me, 2, z * nx + other, True))
            return

        @pl.when(z >= step)
        def _():
            block = me - step * nx
            recv_copy(block)

            @pl.when(z + 1 < nz)
            def _():
                act(copy(block, 4 * step - 1, me + nx))

            act(copy(block, 4 * step, z * nx + other))

        @pl.when(z + step < nz)
        def _():
            block = me + step * nx
            recv_copy(block)

            @pl.when(z >= 1)
            def _():
                act(copy(block, 4 * step + 1, me - nx))

            act(copy(block, 4 * step + 2, z * nx + other))

    def start(c):
        c.start()

    def wait_send(c):
        c.wait_send()

    def nothing(block):
        pass

    def tok_arrive(block):
        tok_copy(block, 0, me).wait_recv()
        core_copy(block).start()

    def core_copy(block):
        return tp_copy(
            tok.at[block, mine],
            tok.at[block, mine],
            tok_csend.at[block],
            tok_crecv.at[block],
            partner,
        )

    def sh_arrive(block):
        sh_copy(block, 0, me).wait_recv()

    gather_moves(tok_copy, nothing, 0, start)

    column = gain[...]
    sh[me, 0] = (sg[...] * column).astype(jnp.bfloat16)
    sh[me, 1] = (su[...] * column).astype(jnp.bfloat16)
    sh[me, 2, 0:rows_d] = sd[:, 0:hw].astype(jnp.bfloat16)
    sh[me, 2, rows_d : 2 * rows_d] = sd[:, hw:dcols].astype(jnp.bfloat16)

    def cast(stage, sendbuf, scaled):
        @pl.loop(0, experts)
        def _(e):
            value = stage[e]
            if scaled:
                value = value * gain[...]
            sendbuf[e] = value.astype(jnp.bfloat16)

    order = [o for o in (6, 4, 2, 7, 5, 3, 1) if o < groups]
    order = order + [o for o in range(1, groups) if o not in order]

    def a2a_ends(index, piece, owner_at, row_at):
        if index < 2:
            sendbuf, recvbuf = ((sb_g, rv_g), (sb_u, rv_u))[index]
            return (
                sendbuf.at[owner_at * per + piece],
                recvbuf.at[piece, pl.ds(row_at * rows_w, rows_w), :],
            )
        columns = pl.ds(piece * hw, hw)
        return (
            sb_d.at[pl.ds(owner_at * per, per), :, columns],
            rv_d.at[:, pl.ds(row_at * rows_d, rows_d), columns],
        )

    def pieces(index):
        return per if index < 2 else 2

    def a2a_copy(index, piece, o):
        target = flip(me, o, groups)
        src, dst = a2a_ends(index, piece, target, me)
        return fs_copy(
            src, dst, a2a_send.at[index, piece, o], a2a_recv.at[index, piece, o], target
        )

    def a2a_own(index, piece):
        src, dst = a2a_ends(index, piece, me, me)
        return pltpu.make_async_copy(src, dst, own_sem.at[index, piece])

    def a2a_start(index, piece):
        for o in order:
            a2a_copy(index, piece, o).start()
        a2a_own(index, piece).start()

    def a2a_arrive(index, piece):
        for o in order:
            a2a_copy(index, piece, o).wait_recv()
        a2a_own(index, piece).wait()

    loads[0].wait()
    cast(st_g, sb_g, True)
    gather_moves(sh_copy, nothing, 0, start)
    gather_moves(tok_copy, tok_arrive, 1, start)
    a2a_start(0, 0)
    loads[1].wait()
    cast(st_u, sb_u, True)
    gather_moves(sh_copy, sh_arrive, 1, start)
    for step in range(2, nz):
        gather_moves(tok_copy, tok_arrive, step, start)
        if step == 2:
            a2a_start(1, 0)
            for piece in range(1, per):
                a2a_start(0, piece)
                a2a_start(1, piece)
            loads[2].wait()
            cast(st_d, sb_d, False)
        gather_moves(sh_copy, sh_arrive, step, start)
    a2a_start(2, 0)
    a2a_start(2, 1)

    for zz in range(nz):
        tok_arrive(zz * nx + (1 - x))
    for zz in range(nz):
        sh_arrive(zz * nx + (1 - x))
    own_tok.wait()

    def sh_out(block, part):
        src_dst = (
            (sh.at[block, 0], out_sg.at[pl.ds(block * rows_w, rows_w), :]),
            (sh.at[block, 1], out_su.at[pl.ds(block * rows_w, rows_w), :]),
            (sh.at[block, 2, pl.ds(0, rows_d)], out_sd.at[pl.ds(block * rows_d, rows_d), pl.ds(0, hw)]),
            (sh.at[block, 2, pl.ds(rows_d, rows_d)], out_sd.at[pl.ds(block * rows_d, rows_d), pl.ds(hw, hw)]),
        )[part]
        return pltpu.make_async_copy(*src_dst, shout_sem.at[block, part])

    for block in range(groups):
        for part in range(4):
            sh_out(block, part).start()

    features = groups * rows_w

    def shared_half(part):
        total = jnp.zeros((tok_count, hcols), jnp.float32)
        for block in range(groups):
            total = total + jnp.dot(
                ext[:, block * rows_w : (block + 1) * rows_w],
                sh[block, part],
                preferred_element_type=jnp.float32,
            )
        return total

    shared_first = shared_half(0)
    shared_second = shared_half(1)
    shid[tp] = (jax.nn.silu(shared_first) * shared_second).astype(jnp.bfloat16)

    def shid_copy(o):
        return tp_copy(
            shid.at[tp], shid.at[tp], shid_send.at[o], shid_recv.at[o], flip(tp, o, ranks)
        )

    def core_arrive(block):
        tp_copy(
            tok.at[block, theirs],
            tok.at[block, theirs],
            tok_csend.at[block],
            tok_crecv.at[block],
            partner,
        ).wait_recv()

    for o in range(1, groups):
        core_arrive(flip(me, o, groups))

    for o in range(1, ranks):
        shid_copy(o).start()

    def hid_core(e, block):
        return tp_copy(
            hid.at[tp, block, e],
            hid.at[tp, block, e],
            hid_csend.at[e, block],
            hid_recv.at[0, e, block],
            partner,
        )

    def hid_across(e, block):
        return tp_copy(
            hid.at[tp, block, e],
            hid.at[tp, block, e],
            hid_ysend.at[e, block],
            hid_recv.at[1, e, block],
            across,
        )

    def hid_forward(e, block):
        return tp_copy(
            hid.at[across, block, e],
            hid.at[across, block, e],
            hid_fsend.at[e, block],
            hid_recv.at[2, e, block],
            partner,
        )

    def turn(o):
        return (me + o) % groups

    def shared_out():
        for o in range(1, ranks):
            shid_copy(o).wait_recv()
        for part in range(2):
            total = jnp.zeros((tok_count, hw), jnp.float32)
            for block in range(groups):
                at = block * rows_d
                total = total + jnp.dot(
                    shid[at // hcols, :, at % hcols : at % hcols + rows_d],
                    sh[block, 2, part * rows_d : (part + 1) * rows_d],
                    preferred_element_type=jnp.float32,
                )
            own_out[:, part * hw : (part + 1) * hw] = total

    for e in range(per):
        a2a_arrive(0, e)
        a2a_arrive(1, e)

        @pl.loop(0, groups)
        def _(o):
            block = turn(o + 1)
            rows = tok[block, :, 0:features]
            first = jnp.dot(rows, rv_g[e], preferred_element_type=jnp.float32)
            second = jnp.dot(rows, rv_u[e], preferred_element_type=jnp.float32)
            hid[tp, block, e] = (jax.nn.silu(first) * second).astype(jnp.bfloat16)

            @pl.when(o >= 1)
            def _():
                before = turn(o)
                hid_across(e, before).start()
                hid_core(e, before).start()

        if e == 0:
            shared_out()
        else:
            hid_across(e - 1, turn(1)).wait_recv()
            hid_forward(e - 1, turn(1)).start()
        hid_across(e, me).start()
        hid_core(e, me).start()

        @pl.loop(0 if e == per - 1 else 1, groups)
        def _(o):
            block = turn(o + 1)
            hid_across(e, block).wait_recv()
            hid_forward(e, block).start()

    @pl.loop(1, groups + 1)
    def _(o):
        block = turn(o)
        for e in range(per):
            hid_core(e, block).wait_recv()
            hid_forward(e, block).wait_recv()

    lanes = lax.broadcasted_iota(jnp.int32, (tok_count, LANES), 1)

    def block_out(block, half_at):
        table = tok[block, :, features : features + LANES].astype(jnp.float32)
        total = jnp.zeros((tok_count, hw), jnp.float32)
        for e in range(per):
            expert = me * per + e
            weight = jnp.sum(
                jnp.where(
                    (lanes == expert) | (lanes == expert + experts) | (lanes == expert + 2 * experts),
                    table,
                    0.0,
                ),
                axis=1,
                keepdims=True,
            )
            out = jnp.zeros((tok_count, hw), jnp.float32)
            for r in range(ranks):
                out = out + jnp.dot(
                    hid[r, block, e],
                    rv_d[e, r * hcols : (r + 1) * hcols, half_at * hw : (half_at + 1) * hw],
                    preferred_element_type=jnp.float32,
                )
            total = total + weight * out
        return total

    def x_copy(part, zz):
        return fs_copy(
            xs.at[part, zz],
            xr.at[part, zz],
            x_send.at[part, zz],
            x_recv.at[part, zz],
            z * nx + (1 - x),
        )

    def z_copy(part, j):
        zz = (z + j) % nz
        return fs_copy(
            zs.at[part, zz], zr.at[part, z], z_send.at[part, j], z_recv.at[part, j], zz * nx + x
        )

    def x_stage(part):
        @pl.loop(1, nz + 1)
        def _(j):
            zz = (z + j) % nz
            xs[part, zz] = block_out(zz * nx + (1 - x), part).astype(jnp.bfloat16)

            @pl.when(j >= 2)
            def _():
                x_copy(part, (z + j - 1) % nz).start()

    def z_stage(part):
        @pl.loop(1, nz + 1)
        def _(j):
            zz = (z + j) % nz
            total = block_out(zz * nx + x, part)

            @pl.when(j == 1)
            def _():
                x_copy(part, z).start()

            x_copy(part, zz).wait_recv()
            total = total + xr[part, zz].astype(jnp.float32)

            @pl.when(j < nz)
            def _():
                zs[part, zz] = total.astype(jnp.bfloat16)

            @pl.when(j == nz)
            def _():
                columns = slice(part * hw, (part + 1) * hw)
                own_out[:, columns] = own_out[:, columns] + total

            @pl.when(j >= 2)
            def _():
                z_copy(part, j - 1).start()

    for part in range(2):
        a2a_arrive(2, part)
        x_stage(part)
        z_stage(part)

    for part in range(2):
        columns = slice(part * hw, (part + 1) * hw)
        for j in range(1, nz):
            z_copy(part, j).wait_recv()
            own_out[:, columns] = own_out[:, columns] + zr[part, (z + nz - j) % nz].astype(jnp.float32)
        out_mixed[:, columns] = own_out[:, columns].astype(jnp.bfloat16)

    for part in range(2):
        for j in range(nz):
            x_copy(part, j).wait_send()
        for j in range(1, nz):
            z_copy(part, j).wait_send()
    for index in range(3):
        for piece in range(pieces(index)):
            for o in order:
                a2a_copy(index, piece, o).wait_send()
    for step in range(nz):
        gather_moves(tok_copy, nothing, step, wait_send)
        gather_moves(sh_copy, nothing, step, wait_send)
    for o in range(1, groups):
        core_copy(flip(me, o, groups)).wait_send()
    for o in range(1, ranks):
        shid_copy(o).wait_send()

    @pl.loop(0, groups)
    def _(o):
        for e in range(per):
            hid_core(e, o).wait_send()
            hid_across(e, o).wait_send()
            hid_forward(e, o).wait_send()

    for block in range(groups):
        for part in range(4):
            sh_out(block, part).wait()


def dense_body(
    tokens,
    norm_gain,
    expert_gate,
    expert_up,
    expert_down,
    shared_gate,
    shared_up,
    shared_down,
    expert_ids,
    route_weights,
):
    groups, ranks = lax.axis_size("fs"), lax.axis_size("tp")
    experts, rows_w, hcols = expert_gate.shape
    rows_d, dcols = expert_down.shape[1:]
    per = experts // groups
    tok_count, features = tokens.shape
    wide = tokens.astype(jnp.float32)
    normed = (wide * lax.rsqrt(jnp.mean(wide * wide, axis=-1, keepdims=True) + EPS)).astype(
        jnp.bfloat16
    )
    named = expert_ids[:, :, None] == jnp.arange(experts, dtype=jnp.int32)[None, None, :]
    table = jnp.sum(jnp.where(named, route_weights[:, :, None], 0.0), axis=1)
    high = lax.reduce_precision(table, 8, 7)
    middle = lax.reduce_precision(table - high, 8, 7)
    low = table - high - middle
    pad = jnp.zeros((tok_count, LANES - 3 * experts), jnp.bfloat16)
    ext = jnp.concatenate(
        [normed] + [v.astype(jnp.bfloat16) for v in (high, middle, low)] + [pad], axis=1
    )
    total = features + LANES
    bf, f32 = jnp.bfloat16, jnp.float32
    dma = pltpu.SemaphoreType.DMA
    nz = groups // 2
    any_space = pl.BlockSpec(memory_space=pl.ANY)
    vmem = pl.BlockSpec(memory_space=pltpu.VMEM)
    hidden = hcols * ranks
    return pl.pallas_call(
        functools.partial(fused_kernel, groups, ranks),
        out_shape=(
            pltpu.VMEM((per, features, hcols), bf),
            pltpu.VMEM((per, features, hcols), bf),
            pltpu.VMEM((per, hidden, dcols), bf),
            pltpu.VMEM((features, hcols), bf),
            pltpu.VMEM((features, hcols), bf),
            pltpu.VMEM((hidden, dcols), bf),
            pltpu.VMEM((tok_count, dcols), bf),
        ),
        in_specs=[vmem, vmem, any_space, any_space, any_space, vmem, vmem, vmem],
        out_specs=(vmem,) * 7,
        scratch_shapes=[
            pltpu.VMEM((experts, rows_w, hcols), f32),
            pltpu.VMEM((experts, rows_w, hcols), f32),
            pltpu.VMEM((experts, rows_d, dcols), f32),
            pltpu.VMEM((experts, rows_w, hcols), bf),
            pltpu.VMEM((experts, rows_w, hcols), bf),
            pltpu.VMEM((experts, rows_d, dcols), bf),
            pltpu.VMEM((groups, 3, rows_w, hcols), bf),
            pltpu.VMEM((groups, tok_count, total), bf),
            pltpu.VMEM((ranks, groups, per, tok_count, hcols), bf),
            pltpu.VMEM((ranks, tok_count, hcols), bf),
            pltpu.VMEM((2, nz, tok_count, dcols // 2), bf),
            pltpu.VMEM((2, nz, tok_count, dcols // 2), bf),
            pltpu.VMEM((2, nz, tok_count, dcols // 2), bf),
            pltpu.VMEM((2, nz, tok_count, dcols // 2), bf),
            pltpu.VMEM((tok_count, dcols), f32),
            dma((3,)),
            dma,
            dma((3, max(per, 2))),
            dma((3, max(per, 2), groups)),
            dma((3, max(per, 2), groups)),
            dma((4 * nz,)),
            dma((groups,)),
            dma((groups,)),
            dma((groups,)),
            dma((4 * nz,)),
            dma((groups,)),
            dma((per, groups)),
            dma((per, groups)),
            dma((per, groups)),
            dma((3, per, groups)),
            dma((ranks,)),
            dma((ranks,)),
            dma((2, nz)),
            dma((2, nz)),
            dma((2, nz)),
            dma((2, nz)),
            dma((groups, 4)),
        ],
        compiler_params=pltpu.CompilerParams(
            collective_id=0, has_side_effects=True, vmem_limit_bytes=VMEM_BYTES
        ),
    )(
        ext,
        norm_gain[:, None],
        expert_gate,
        expert_up,
        expert_down,
        shared_gate,
        shared_up,
        shared_down,
    )


def expert_hidden(rows, gate_new, up_new):
    first = jnp.einsum("secn,enf->secf", rows, gate_new, preferred_element_type=jnp.float32)
    second = jnp.einsum("secn,enf->secf", rows, up_new, preferred_element_type=jnp.float32)
    return (jax.nn.silu(first) * second).astype(jnp.bfloat16)


def body(
    tokens,
    norm_gain,
    expert_gate,
    expert_up,
    expert_down,
    shared_gate,
    shared_up,
    shared_down,
    expert_ids,
    route_weights,
):
    groups = lax.axis_size("fs")
    experts = expert_gate.shape[0]
    per_group = experts // groups
    tok_count = tokens.shape[0]
    capacity = 2 * tok_count * TOP_K // experts
    ranks = lax.axis_size("tp")
    square = expert_down.shape[1] * expert_down.shape[2] == shared_gate.size
    if capacity >= tok_count and groups & (groups - 1) == 0 and ranks == 4 and square:
        return dense_body(
            tokens,
            norm_gain,
            expert_gate,
            expert_up,
            expert_down,
            shared_gate,
            shared_up,
            shared_down,
            expert_ids,
            route_weights,
        )
    gate_local = (expert_gate * norm_gain[None, :, None]).astype(jnp.bfloat16)
    up_local = (expert_up * norm_gain[None, :, None]).astype(jnp.bfloat16)
    down_local = expert_down.astype(jnp.bfloat16)
    gate_local = gate_local.reshape((groups, per_group) + gate_local.shape[1:])
    up_local = up_local.reshape((groups, per_group) + up_local.shape[1:])
    down_local = down_local.reshape((groups, per_group) + down_local.shape[1:])
    shared_first_local = (shared_gate * norm_gain[:, None]).astype(jnp.bfloat16)
    shared_second_local = (shared_up * norm_gain[:, None]).astype(jnp.bfloat16)
    shared_third_local = shared_down.astype(jnp.bfloat16)
    gate_moved, up_moved, down_moved = (
        lax.all_to_all(gate_local, "fs", split_axis=0, concat_axis=2, tiled=True),
        lax.all_to_all(up_local, "fs", split_axis=0, concat_axis=2, tiled=True),
        lax.all_to_all(down_local, "fs", split_axis=0, concat_axis=2, tiled=True),
    )
    down_ready = down_moved[0]
    gate_ready = gate_moved[0]
    up_ready = up_moved[0]
    shared_gate_ready, shared_up_ready, shared_down_ready = (
        lax.all_gather(shared_first_local, "fs", axis=0, tiled=True),
        lax.all_gather(shared_second_local, "fs", axis=0, tiled=True),
        lax.all_gather(shared_third_local, "fs", axis=0, tiled=True),
    )
    wide = tokens.astype(jnp.float32)
    normed = (wide * lax.rsqrt(jnp.mean(wide * wide, axis=-1, keepdims=True) + EPS)).astype(
        jnp.bfloat16
    )
    chosen = expert_ids.reshape(-1)
    onehot = (chosen[:, None] == jnp.arange(experts, dtype=jnp.int32)[None, :]).astype(jnp.int32)
    ranks = jnp.sum(jnp.cumsum(onehot, axis=0) * onehot, axis=1) - 1
    owners = jnp.arange(tok_count * TOP_K, dtype=jnp.int32) // TOP_K
    slot_token = jnp.zeros((experts, capacity), jnp.int32).at[chosen, ranks].set(owners)
    outgoing = normed[slot_token.reshape(-1)].reshape(groups, per_group, capacity, normed.shape[1])
    share = capacity // lax.axis_size("tp")
    mine = lax.dynamic_slice_in_dim(outgoing, lax.axis_index("tp") * share, share, 2)
    arrived = lax.all_to_all(mine, "fs", split_axis=0, concat_axis=0, tiled=True)
    hidden = expert_hidden(lax.all_gather(arrived, "tp", axis=2, tiled=True), gate_ready, up_ready)
    shared_first = jnp.dot(normed, shared_gate_ready, preferred_element_type=jnp.float32)
    shared_second = jnp.dot(normed, shared_up_ready, preferred_element_type=jnp.float32)
    shared_hidden = (jax.nn.silu(shared_first) * shared_second).astype(jnp.bfloat16)[None, None]
    columns = down_ready.shape[2]
    routed_piece = lax.all_gather(hidden, "tp", axis=3, tiled=True)
    shared_piece = lax.all_gather(shared_hidden, "tp", axis=3, tiled=True)
    routed_total = jnp.einsum(
        "secf,efd->secd", routed_piece, down_ready, preferred_element_type=jnp.float32
    )
    shared_total = jnp.einsum(
        "abtf,fd->abtd", shared_piece, shared_down_ready, preferred_element_type=jnp.float32
    )
    returned = lax.all_to_all(
        routed_total.astype(jnp.bfloat16), "fs", split_axis=0, concat_axis=0, tiled=True
    )
    returned = returned.reshape(experts * capacity, columns)
    picked = (
        returned[chosen * capacity + ranks].astype(jnp.float32).reshape(tok_count, TOP_K, columns)
    )
    routed = jnp.sum(picked * route_weights[:, :, None], axis=1)
    mixed = (shared_total[0, 0] + routed).astype(jnp.bfloat16)
    return (
        gate_ready,
        up_ready,
        down_ready,
        shared_gate_ready,
        shared_up_ready,
        shared_down_ready,
        mixed,
    )


def solution(mesh):
    in_specs = (
        P("fs", None),
        P("fs"),
        P(None, "fs", "tp"),
        P(None, "fs", "tp"),
        P(None, "fs", "tp"),
        P("fs", "tp"),
        P("fs", "tp"),
        P("fs", "tp"),
        P("fs", None),
        P("fs", None),
    )
    out_specs = (
        P("fs", None, "tp"),
        P("fs", None, "tp"),
        P("fs", None, "tp"),
        P(None, "tp"),
        P(None, "tp"),
        P(None, "tp"),
        P("fs", "tp"),
    )
    return jax.shard_map(body, mesh=mesh, in_specs=in_specs, out_specs=out_specs, check_vma=False)
```

```python
import functools
import jax
import jax.numpy as jnp
from jax import lax
from jax.experimental import pallas as pl
from jax.experimental.pallas import tpu as pltpu
from jax.sharding import PartitionSpec as P

TOP_K = 8


EPS = 1e-06

MESH = pl.DeviceIdType.MESH
LANES = 128
VMEM_BYTES = 48 * 1024 * 1024


def flip(value, mask, extent):
    result, bit = 0, 1
    while bit < extent:
        digit = (value // bit) % 2
        result = result + bit * ((1 - digit) if mask & bit else digit)
        bit *= 2
    return result


def fused_kernel(
    groups,
    ranks,
    ext,
    gain,
    eg,
    eu,
    ed,
    sg,
    su,
    sd,
    rv_g,
    rv_u,
    rv_d,
    out_sg,
    out_su,
    out_sd,
    out_mixed,
    st_g,
    st_u,
    st_d,
    sb_g,
    sb_u,
    sb_d,
    sh,
    tok,
    hid,
    shid,
    xs,
    xr,
    zs,
    zr,
    own_out,
    load_sem,
    loc_sem,
    own_sem,
    a2a_send,
    a2a_recv,
    tok_send,
    tok_recv,
    tok_tsend,
    tok_trecv,
    sh_send,
    sh_recv,
    hid_csend,
    hid_ysend,
    hid_fsend,
    hid_recv,
    shid_send,
    shid_recv,
    x_send,
    x_recv,
    z_send,
    z_recv,
    shout_sem,
):
    nx = 2
    nz = groups // nx
    me = lax.axis_index("fs")
    tp = lax.axis_index("tp")
    z, x = me // nx, me % nx
    partner = flip(tp, 1, ranks)
    across = flip(tp, 2, ranks)
    per = eg.shape[0] // groups
    experts = eg.shape[0]
    rows_w = eg.shape[1]
    rows_d = ed.shape[1]
    tok_count = ext.shape[0]
    width = st_d.shape[2] * ranks
    share = tok_count // ranks
    hcols = eg.shape[2]
    dcols = ed.shape[2]
    hw = dcols // 2

    loads = [
        pltpu.make_async_copy(a, b, load_sem.at[i])
        for i, (a, b) in enumerate(((eg, st_g), (eu, st_u), (ed, st_d)))
    ]
    for load in loads:
        load.start()
    own_tok = pltpu.make_async_copy(ext, tok.at[me], loc_sem)
    own_tok.start()

    barrier = pltpu.get_barrier_semaphore()
    for o in range(1, groups):
        pl.semaphore_signal(
            barrier, inc=1, device_id={"fs": flip(me, o, groups)}, device_id_type=MESH
        )
    for o in range(1, ranks):
        pl.semaphore_signal(
            barrier, inc=1, device_id={"tp": flip(tp, o, ranks)}, device_id_type=MESH
        )
    pl.semaphore_wait(barrier, groups + ranks - 2)

    mine = pl.ds(tp * share, share)
    theirs = pl.ds(across * share, share)

    def fs_copy(src, dst, send, recv, target):
        return pltpu.make_async_remote_copy(
            src_ref=src,
            dst_ref=dst,
            send_sem=send,
            recv_sem=recv,
            device_id={"fs": target},
            device_id_type=MESH,
        )

    def tp_copy(src, dst, send, recv, target):
        return pltpu.make_async_remote_copy(
            src_ref=src,
            dst_ref=dst,
            send_sem=send,
            recv_sem=recv,
            device_id={"tp": target},
            device_id_type=MESH,
        )

    def tok_copy(block, slot, target, own=False):
        src = ext.at[mine] if own else tok.at[block, mine]
        return fs_copy(src, tok.at[block, mine], tok_send.at[slot], tok_recv.at[block], target)

    def sh_copy(block, slot, target, own=False):
        return fs_copy(sh.at[block], sh.at[block], sh_send.at[slot], sh_recv.at[block], target)

    def gather_moves(copy, recv_copy, step, act):
        other = 1 - x
        if step == 0:

            @pl.when(z + 1 < nz)
            def _():
                act(copy(me, 0, me + nx, True))

            @pl.when(z >= 1)
            def _():
                act(copy(me, 1, me - nx, True))

            act(copy(me, 2, z * nx + other, True))
            return

        @pl.when(z >= step)
        def _():
            block = me - step * nx
            recv_copy(block)

            @pl.when(z + 1 < nz)
            def _():
                act(copy(block, 4 * step - 1, me + nx))

            act(copy(block, 4 * step, z * nx + other))

        @pl.when(z + step < nz)
        def _():
            block = me + step * nx
            recv_copy(block)

            @pl.when(z >= 1)
            def _():
                act(copy(block, 4 * step + 1, me - nx))

            act(copy(block, 4 * step + 2, z * nx + other))

    def start(c):
        c.start()

    def wait_send(c):
        c.wait_send()

    def nothing(block):
        pass

    def tok_arrive(block):
        tok_copy(block, 0, me).wait_recv()
        tok_share(0, block).start()
        tok_share(1, block).start()

    def tok_share(kind, block):
        rows = theirs if kind == 2 else mine
        return tp_copy(
            tok.at[block, rows],
            tok.at[block, rows],
            tok_tsend.at[kind, block],
            tok_trecv.at[kind, block],
            across if kind == 1 else partner,
        )

    def sh_arrive(block):
        sh_copy(block, 0, me).wait_recv()

    gather_moves(tok_copy, nothing, 0, start)

    column = gain[...]
    sh[me, 0] = (sg[...] * column).astype(jnp.bfloat16)
    sh[me, 1] = (su[...] * column).astype(jnp.bfloat16)
    sh[me, 2, 0:rows_d] = sd[:, 0:hw].astype(jnp.bfloat16)
    sh[me, 2, rows_d : 2 * rows_d] = sd[:, hw:dcols].astype(jnp.bfloat16)

    def cast(stage, sendbuf, scaled):
        @pl.loop(0, experts)
        def _(e):
            value = stage[e]
            if scaled:
                value = value * gain[...]
            sendbuf[e] = value.astype(jnp.bfloat16)

    order = [o for o in (7, 5, 6, 4, 3, 2, 1) if o < groups]
    order = order + [o for o in range(1, groups) if o not in order]

    def a2a_ends(index, piece, owner_at, row_at):
        if index < 2:
            sendbuf, recvbuf = ((sb_g, rv_g), (sb_u, rv_u))[index]
            return (
                sendbuf.at[owner_at * per + piece],
                recvbuf.at[piece, pl.ds(row_at * rows_w, rows_w), :],
            )
        columns = pl.ds(piece * hw, hw)
        return (
            sb_d.at[pl.ds(owner_at * per, per), :, columns],
            rv_d.at[:, pl.ds(row_at * rows_d, rows_d), columns],
        )

    def pieces(index):
        return per if index < 2 else 2

    def a2a_copy(index, piece, o):
        target = flip(me, o, groups)
        src, dst = a2a_ends(index, piece, target, me)
        return fs_copy(
            src, dst, a2a_send.at[index, piece, o], a2a_recv.at[index, piece, o], target
        )

    def a2a_own(index, piece):
        src, dst = a2a_ends(index, piece, me, me)
        return pltpu.make_async_copy(src, dst, own_sem.at[index, piece])

    def a2a_start(index, piece):
        for o in order:
            a2a_copy(index, piece, o).start()
        a2a_own(index, piece).start()

    def a2a_arrive(index, piece):
        for o in order:
            a2a_copy(index, piece, o).wait_recv()
        a2a_own(index, piece).wait()

    loads[0].wait()
    cast(st_g, sb_g, True)
    gather_moves(sh_copy, nothing, 0, start)
    gather_moves(tok_copy, tok_arrive, 1, start)
    a2a_start(0, 0)
    loads[1].wait()
    cast(st_u, sb_u, True)
    for step in range(2, nz):
        gather_moves(tok_copy, tok_arrive, step, start)
        if step == 2:
            a2a_start(1, 0)
            loads[2].wait()
            cast(st_d, sb_d, False)
            gather_moves(sh_copy, sh_arrive, 1, start)

    for zz in range(nz):
        tok_arrive(zz * nx + (1 - x))
    own_tok.wait()
    for o in range(1, groups):
        tok_share(1, flip(me, o, groups)).wait_recv()
        tok_share(2, flip(me, o, groups)).start()
    for piece in range(1, per):
        a2a_start(0, piece)
        a2a_start(1, piece)
    for step in range(2, nz - 1):
        gather_moves(sh_copy, sh_arrive, step, start)

    def sh_out(block, part):
        src_dst = (
            (sh.at[block, 0], out_sg.at[pl.ds(block * rows_w, rows_w), :]),
            (sh.at[block, 1], out_su.at[pl.ds(block * rows_w, rows_w), :]),
            (sh.at[block, 2, pl.ds(0, rows_d)], out_sd.at[pl.ds(block * rows_d, rows_d), pl.ds(0, hw)]),
            (sh.at[block, 2, pl.ds(rows_d, rows_d)], out_sd.at[pl.ds(block * rows_d, rows_d), pl.ds(hw, hw)]),
        )[part]
        return pltpu.make_async_copy(*src_dst, shout_sem.at[block, part])

    features = groups * rows_w

    def shared_half(part):
        total = jnp.zeros((tok_count, hcols), jnp.float32)
        for block in range(groups):
            total = total + jnp.dot(
                ext[:, block * rows_w : (block + 1) * rows_w],
                sh[block, part],
                preferred_element_type=jnp.float32,
            )
        return total

    def shared_hidden():
        for zz in range(nz):
            sh_arrive(zz * nx + (1 - x))
        for block in range(groups):
            for part in range(4):
                sh_out(block, part).start()
        first = shared_half(0)
        second = shared_half(1)
        shid[tp] = (jax.nn.silu(first) * second).astype(jnp.bfloat16)

    def shid_copy(o):
        return tp_copy(
            shid.at[tp], shid.at[tp], shid_send.at[o], shid_recv.at[o], flip(tp, o, ranks)
        )

    for o in range(1, groups):
        tok_share(0, flip(me, o, groups)).wait_recv()
        tok_share(2, flip(me, o, groups)).wait_recv()

    def hid_core(e, block):
        return tp_copy(
            hid.at[tp, block, e],
            hid.at[tp, block, e],
            hid_csend.at[e, block],
            hid_recv.at[0, e, block],
            partner,
        )

    def hid_across(e, block):
        return tp_copy(
            hid.at[tp, block, e],
            hid.at[tp, block, e],
            hid_ysend.at[e, block],
            hid_recv.at[1, e, block],
            across,
        )

    def hid_forward(e, block):
        return tp_copy(
            hid.at[across, block, e],
            hid.at[across, block, e],
            hid_fsend.at[e, block],
            hid_recv.at[2, e, block],
            partner,
        )

    def turn(o):
        return (me + o) % groups

    def shared_out():
        for o in range(1, ranks):
            shid_copy(o).wait_recv()
        for part in range(2):
            total = jnp.zeros((tok_count, hw), jnp.float32)
            for block in range(groups):
                at = block * rows_d
                total = total + jnp.dot(
                    shid[at // hcols, :, at % hcols : at % hcols + rows_d],
                    sh[block, 2, part * rows_d : (part + 1) * rows_d],
                    preferred_element_type=jnp.float32,
                )
            own_out[:, part * hw : (part + 1) * hw] = total

    for e in range(per):
        a2a_arrive(0, e)
        a2a_arrive(1, e)
        if e == 0:
            a2a_start(2, 0)
            a2a_start(2, 1)

        @pl.loop(0, groups)
        def _(o):
            block = turn(o + 1)
            rows = tok[block, :, 0:features]
            first = jnp.dot(rows, rv_g[e], preferred_element_type=jnp.float32)
            second = jnp.dot(rows, rv_u[e], preferred_element_type=jnp.float32)
            hid[tp, block, e] = (jax.nn.silu(first) * second).astype(jnp.bfloat16)

            @pl.when(o >= 1)
            def _():
                before = turn(o)
                hid_across(e, before).start()
                hid_core(e, before).start()

        if e > 0:
            hid_across(e - 1, turn(1)).wait_recv()
            hid_forward(e - 1, turn(1)).start()
        if e == per - 1:
            shared_hidden()
        hid_across(e, me).start()
        hid_core(e, me).start()

        @pl.loop(0 if e == per - 1 else 1, groups)
        def _(o):
            block = turn(o + 1)
            hid_across(e, block).wait_recv()
            hid_forward(e, block).start()

        if e == 0:
            gather_moves(sh_copy, sh_arrive, nz - 1, start)
        if e == per - 1:
            for o in range(1, ranks):
                shid_copy(o).start()

    shared_out()

    @pl.loop(1, groups + 1)
    def _(o):
        block = turn(o)
        for e in range(per):
            hid_core(e, block).wait_recv()
            hid_forward(e, block).wait_recv()

    lanes = lax.broadcasted_iota(jnp.int32, (tok_count, LANES), 1)

    def block_out(block, half_at):
        table = tok[block, :, features : features + LANES].astype(jnp.float32)
        total = jnp.zeros((tok_count, hw), jnp.float32)
        for e in range(per):
            expert = me * per + e
            weight = jnp.sum(
                jnp.where(
                    (lanes == expert) | (lanes == expert + experts) | (lanes == expert + 2 * experts),
                    table,
                    0.0,
                ),
                axis=1,
                keepdims=True,
            )
            out = jnp.zeros((tok_count, hw), jnp.float32)
            for r in range(ranks):
                out = out + jnp.dot(
                    hid[r, block, e],
                    rv_d[e, r * hcols : (r + 1) * hcols, half_at * hw : (half_at + 1) * hw],
                    preferred_element_type=jnp.float32,
                )
            total = total + weight * out
        return total

    def x_copy(part, zz):
        return fs_copy(
            xs.at[part, zz],
            xr.at[part, zz],
            x_send.at[part, zz],
            x_recv.at[part, zz],
            z * nx + (1 - x),
        )

    def z_copy(part, j):
        zz = (z + j) % nz
        return fs_copy(
            zs.at[part, zz], zr.at[part, z], z_send.at[part, j], z_recv.at[part, j], zz * nx + x
        )

    def x_stage(part):
        @pl.loop(1, nz + 1)
        def _(j):
            zz = (z + j) % nz
            xs[part, zz] = block_out(zz * nx + (1 - x), part).astype(jnp.bfloat16)

            @pl.when(j >= 2)
            def _():
                x_copy(part, (z + j - 1) % nz).start()

    def z_stage(part):
        @pl.loop(1, nz + 1)
        def _(j):
            zz = (z + j) % nz
            total = block_out(zz * nx + x, part)

            @pl.when(j == 1)
            def _():
                x_copy(part, z).start()

            x_copy(part, zz).wait_recv()
            total = total + xr[part, zz].astype(jnp.float32)

            @pl.when(j < nz)
            def _():
                zs[part, zz] = total.astype(jnp.bfloat16)

            @pl.when(j == nz)
            def _():
                columns = slice(part * hw, (part + 1) * hw)
                own_out[:, columns] = own_out[:, columns] + total

            @pl.when(j >= 2)
            def _():
                z_copy(part, j - 1).start()

    for part in range(2):
        a2a_arrive(2, part)
        x_stage(part)
        z_stage(part)

    for part in range(2):
        columns = slice(part * hw, (part + 1) * hw)
        for j in range(1, nz):
            z_copy(part, j).wait_recv()
            own_out[:, columns] = own_out[:, columns] + zr[part, (z + nz - j) % nz].astype(jnp.float32)
        out_mixed[:, columns] = own_out[:, columns].astype(jnp.bfloat16)

    for part in range(2):
        for j in range(nz):
            x_copy(part, j).wait_send()
        for j in range(1, nz):
            z_copy(part, j).wait_send()
    for index in range(3):
        for piece in range(pieces(index)):
            for o in order:
                a2a_copy(index, piece, o).wait_send()
    for step in range(nz):
        gather_moves(tok_copy, nothing, step, wait_send)
        gather_moves(sh_copy, nothing, step, wait_send)
    for o in range(1, groups):
        for kind in range(3):
            tok_share(kind, flip(me, o, groups)).wait_send()
    for o in range(1, ranks):
        shid_copy(o).wait_send()

    @pl.loop(0, groups)
    def _(o):
        for e in range(per):
            hid_core(e, o).wait_send()
            hid_across(e, o).wait_send()
            hid_forward(e, o).wait_send()

    for block in range(groups):
        for part in range(4):
            sh_out(block, part).wait()


def dense_body(
    tokens,
    norm_gain,
    expert_gate,
    expert_up,
    expert_down,
    shared_gate,
    shared_up,
    shared_down,
    expert_ids,
    route_weights,
):
    groups, ranks = lax.axis_size("fs"), lax.axis_size("tp")
    experts, rows_w, hcols = expert_gate.shape
    rows_d, dcols = expert_down.shape[1:]
    per = experts // groups
    tok_count, features = tokens.shape
    wide = tokens.astype(jnp.float32)
    normed = (wide * lax.rsqrt(jnp.mean(wide * wide, axis=-1, keepdims=True) + EPS)).astype(
        jnp.bfloat16
    )
    named = expert_ids[:, :, None] == jnp.arange(experts, dtype=jnp.int32)[None, None, :]
    table = jnp.sum(jnp.where(named, route_weights[:, :, None], 0.0), axis=1)
    high = lax.reduce_precision(table, 8, 7)
    middle = lax.reduce_precision(table - high, 8, 7)
    low = table - high - middle
    pad = jnp.zeros((tok_count, LANES - 3 * experts), jnp.bfloat16)
    ext = jnp.concatenate(
        [normed] + [v.astype(jnp.bfloat16) for v in (high, middle, low)] + [pad], axis=1
    )
    total = features + LANES
    bf, f32 = jnp.bfloat16, jnp.float32
    dma = pltpu.SemaphoreType.DMA
    nz = groups // 2
    any_space = pl.BlockSpec(memory_space=pl.ANY)
    vmem = pl.BlockSpec(memory_space=pltpu.VMEM)
    hidden = hcols * ranks
    return pl.pallas_call(
        functools.partial(fused_kernel, groups, ranks),
        out_shape=(
            pltpu.VMEM((per, features, hcols), bf),
            pltpu.VMEM((per, features, hcols), bf),
            pltpu.VMEM((per, hidden, dcols), bf),
            pltpu.VMEM((features, hcols), bf),
            pltpu.VMEM((features, hcols), bf),
            pltpu.VMEM((hidden, dcols), bf),
            pltpu.VMEM((tok_count, dcols), bf),
        ),
        in_specs=[vmem, vmem, any_space, any_space, any_space, vmem, vmem, vmem],
        out_specs=(vmem,) * 7,
        scratch_shapes=[
            pltpu.VMEM((experts, rows_w, hcols), f32),
            pltpu.VMEM((experts, rows_w, hcols), f32),
            pltpu.VMEM((experts, rows_d, dcols), f32),
            pltpu.VMEM((experts, rows_w, hcols), bf),
            pltpu.VMEM((experts, rows_w, hcols), bf),
            pltpu.VMEM((experts, rows_d, dcols), bf),
            pltpu.VMEM((groups, 3, rows_w, hcols), bf),
            pltpu.VMEM((groups, tok_count, total), bf),
            pltpu.VMEM((ranks, groups, per, tok_count, hcols), bf),
            pltpu.VMEM((ranks, tok_count, hcols), bf),
            pltpu.VMEM((2, nz, tok_count, dcols // 2), bf),
            pltpu.VMEM((2, nz, tok_count, dcols // 2), bf),
            pltpu.VMEM((2, nz, tok_count, dcols // 2), bf),
            pltpu.VMEM((2, nz, tok_count, dcols // 2), bf),
            pltpu.VMEM((tok_count, dcols), f32),
            dma((3,)),
            dma,
            dma((3, max(per, 2))),
            dma((3, max(per, 2), groups)),
            dma((3, max(per, 2), groups)),
            dma((4 * nz,)),
            dma((groups,)),
            dma((3, groups)),
            dma((3, groups)),
            dma((4 * nz,)),
            dma((groups,)),
            dma((per, groups)),
            dma((per, groups)),
            dma((per, groups)),
            dma((3, per, groups)),
            dma((ranks,)),
            dma((ranks,)),
            dma((2, nz)),
            dma((2, nz)),
            dma((2, nz)),
            dma((2, nz)),
            dma((groups, 4)),
        ],
        compiler_params=pltpu.CompilerParams(
            collective_id=0, has_side_effects=True, vmem_limit_bytes=VMEM_BYTES
        ),
    )(
        ext,
        norm_gain[:, None],
        expert_gate,
        expert_up,
        expert_down,
        shared_gate,
        shared_up,
        shared_down,
    )


def expert_hidden(rows, gate_new, up_new):
    first = jnp.einsum("secn,enf->secf", rows, gate_new, preferred_element_type=jnp.float32)
    second = jnp.einsum("secn,enf->secf", rows, up_new, preferred_element_type=jnp.float32)
    return (jax.nn.silu(first) * second).astype(jnp.bfloat16)


def body(
    tokens,
    norm_gain,
    expert_gate,
    expert_up,
    expert_down,
    shared_gate,
    shared_up,
    shared_down,
    expert_ids,
    route_weights,
):
    groups = lax.axis_size("fs")
    experts = expert_gate.shape[0]
    per_group = experts // groups
    tok_count = tokens.shape[0]
    capacity = 2 * tok_count * TOP_K // experts
    ranks = lax.axis_size("tp")
    square = expert_down.shape[1] * expert_down.shape[2] == shared_gate.size
    if capacity >= tok_count and per_group >= 2 and groups >= 8 and groups & (groups - 1) == 0 and ranks == 4 and square:
        return dense_body(
            tokens,
            norm_gain,
            expert_gate,
            expert_up,
            expert_down,
            shared_gate,
            shared_up,
            shared_down,
            expert_ids,
            route_weights,
        )
    gate_local = (expert_gate * norm_gain[None, :, None]).astype(jnp.bfloat16)
    up_local = (expert_up * norm_gain[None, :, None]).astype(jnp.bfloat16)
    down_local = expert_down.astype(jnp.bfloat16)
    gate_local = gate_local.reshape((groups, per_group) + gate_local.shape[1:])
    up_local = up_local.reshape((groups, per_group) + up_local.shape[1:])
    down_local = down_local.reshape((groups, per_group) + down_local.shape[1:])
    shared_first_local = (shared_gate * norm_gain[:, None]).astype(jnp.bfloat16)
    shared_second_local = (shared_up * norm_gain[:, None]).astype(jnp.bfloat16)
    shared_third_local = shared_down.astype(jnp.bfloat16)
    gate_moved, up_moved, down_moved = (
        lax.all_to_all(gate_local, "fs", split_axis=0, concat_axis=2, tiled=True),
        lax.all_to_all(up_local, "fs", split_axis=0, concat_axis=2, tiled=True),
        lax.all_to_all(down_local, "fs", split_axis=0, concat_axis=2, tiled=True),
    )
    down_ready = down_moved[0]
    gate_ready = gate_moved[0]
    up_ready = up_moved[0]
    shared_gate_ready, shared_up_ready, shared_down_ready = (
        lax.all_gather(shared_first_local, "fs", axis=0, tiled=True),
        lax.all_gather(shared_second_local, "fs", axis=0, tiled=True),
        lax.all_gather(shared_third_local, "fs", axis=0, tiled=True),
    )
    wide = tokens.astype(jnp.float32)
    normed = (wide * lax.rsqrt(jnp.mean(wide * wide, axis=-1, keepdims=True) + EPS)).astype(
        jnp.bfloat16
    )
    chosen = expert_ids.reshape(-1)
    onehot = (chosen[:, None] == jnp.arange(experts, dtype=jnp.int32)[None, :]).astype(jnp.int32)
    ranks = jnp.sum(jnp.cumsum(onehot, axis=0) * onehot, axis=1) - 1
    owners = jnp.arange(tok_count * TOP_K, dtype=jnp.int32) // TOP_K
    slot_token = jnp.zeros((experts, capacity), jnp.int32).at[chosen, ranks].set(owners)
    outgoing = normed[slot_token.reshape(-1)].reshape(groups, per_group, capacity, normed.shape[1])
    share = capacity // lax.axis_size("tp")
    mine = lax.dynamic_slice_in_dim(outgoing, lax.axis_index("tp") * share, share, 2)
    arrived = lax.all_to_all(mine, "fs", split_axis=0, concat_axis=0, tiled=True)
    hidden = expert_hidden(lax.all_gather(arrived, "tp", axis=2, tiled=True), gate_ready, up_ready)
    shared_first = jnp.dot(normed, shared_gate_ready, preferred_element_type=jnp.float32)
    shared_second = jnp.dot(normed, shared_up_ready, preferred_element_type=jnp.float32)
    shared_hidden = (jax.nn.silu(shared_first) * shared_second).astype(jnp.bfloat16)[None, None]
    columns = down_ready.shape[2]
    routed_piece = lax.all_gather(hidden, "tp", axis=3, tiled=True)
    shared_piece = lax.all_gather(shared_hidden, "tp", axis=3, tiled=True)
    routed_total = jnp.einsum(
        "secf,efd->secd", routed_piece, down_ready, preferred_element_type=jnp.float32
    )
    shared_total = jnp.einsum(
        "abtf,fd->abtd", shared_piece, shared_down_ready, preferred_element_type=jnp.float32
    )
    returned = lax.all_to_all(
        routed_total.astype(jnp.bfloat16), "fs", split_axis=0, concat_axis=0, tiled=True
    )
    returned = returned.reshape(experts * capacity, columns)
    picked = (
        returned[chosen * capacity + ranks].astype(jnp.float32).reshape(tok_count, TOP_K, columns)
    )
    routed = jnp.sum(picked * route_weights[:, :, None], axis=1)
    mixed = (shared_total[0, 0] + routed).astype(jnp.bfloat16)
    return (
        gate_ready,
        up_ready,
        down_ready,
        shared_gate_ready,
        shared_up_ready,
        shared_down_ready,
        mixed,
    )


def solution(mesh):
    in_specs = (
        P("fs", None),
        P("fs"),
        P(None, "fs", "tp"),
        P(None, "fs", "tp"),
        P(None, "fs", "tp"),
        P("fs", "tp"),
        P("fs", "tp"),
        P("fs", "tp"),
        P("fs", None),
        P("fs", None),
    )
    out_specs = (
        P("fs", None, "tp"),
        P("fs", None, "tp"),
        P("fs", None, "tp"),
        P(None, "tp"),
        P(None, "tp"),
        P(None, "tp"),
        P("fs", "tp"),
    )
    return jax.shard_map(body, mesh=mesh, in_specs=in_specs, out_specs=out_specs, check_vma=False)
```
